32 devices in a mesh: gr: 2 (over x), sp: 8 (over z, y), tp: 2 (over core).
Axes of the slice: x: 2, y: 2, z: 4, core: 2. Of those that a mesh axis runs over, the one named last changes fastest.
Arguments:
- tokens: bfloat16 [8, 2048, 2048], P('gr', 'sp'), parts along dimension 0, may hold values from -6 to 6
- new_rows: bfloat16 [8, 2048], P('gr'), parts along dimension 0, may hold values from -6 to 6
- new_query: bfloat16 [8, 1024], P('gr', 'tp'), parts along dimension 0, may hold values from -6 to 6
- norm_gain: bfloat16 [2048], replicated, may hold values from 0.099609375 to 1.8984375
- key_weight: bfloat16 [2048, 1024], P('sp', 'tp'), may hold values from -0.125 to 0.125
- value_weight: bfloat16 [2048, 2048], P('sp', 'tp'), may hold values from -0.125 to 0.125
- input_weight: bfloat16 [2048, 16], replicated, may hold values from -0.125 to 0.125
- forget_weight: bfloat16 [2048, 16], replicated, may hold values from -0.125 to 0.125
- forget_bias: float32 [16], P('tp'), may hold values from 3 to 12
- gate_offsets: float32 [8, 2048, 2, 16], P('gr', 'sp', None, 'tp'), parts along dimension 0, may hold values from -6 to 250, as said below
Outputs:
- cache_keys: bfloat16 [16, 1024, 1024], P(('gr', 'sp'), None, 'tp'), parts along dimension 0
- cache_values: bfloat16 [16, 1024, 2048], P(('gr', 'sp'), None, 'tp'), parts along dimension 0
- cache_weights: float32 [16, 16, 1024], P(('gr', 'sp'), 'tp'), parts along dimension 0
- first_read: bfloat16 [8, 2048], P('gr', 'tp'), parts along dimension 0
The draws below stay inside these ranges and needn't reach their ends.
There are 2 independent parts, one for each index of `gr`. The reference program is written for one: setup_inputs(seed, part) draws one part's arguments, and reference() takes and returns one part's arrays. A program takes and returns all parts, laid end to end along the dimension named above; an argument that names none is the same for every part. Nothing has to cross between parts.
Inputs may be any that keep to these rules, and one draw needn't show every extreme that they name: `gate_offsets`: entry 1 along the third dimension is never positive.
All inputs are finite; a program needn't handle non-finite values.
Results may differ from the reference program's by a relative error of at most 0.012.
The reference program's roundings to bfloat16 on the way count: a program that leaves them out, or rounds other values in their place, can miss the bound.
Values may be sent and summed in bfloat16 or wider, within the bound.
A program may use at most 64 MiB of HBM per device.

```python
import math
import jax
import jax.numpy as jnp
from jax import lax

D = 2048
HEADS = 16
DK = 64
DV = 128
SEQS = 4
CONTEXT_SPAN = 2048
PIECES = 2
SUB = 128
N_SP = 8


def draw_forget_bias(key, part):
    pick_key, slow_key, fast_key = jax.random.split(key, 3)
    fast_share = 0.5
    is_fast = jax.random.uniform(pick_key, (HEADS,), jnp.float32) < fast_share
    slow_bias = math.log(3.3 * CONTEXT_SPAN) + jax.random.uniform(slow_key, (HEADS,), jnp.float32, -0.3, 0.3)
    fast_bias = math.log(60.0) + jax.random.uniform(fast_key, (HEADS,), jnp.float32, -0.5, 0.5)
    return jnp.where(is_fast, fast_bias, slow_bias).astype(jnp.float32)


def draw_gate_offsets(key, part):
    incomplete_key_vectors = jax.random.split(key, 4)
    tensor_dimension_count = (SEQS, CONTEXT_SPAN, HEADS)
    block_rate = jnp.exp(jax.random.uniform(incomplete_key_vectors[0], (SEQS, CONTEXT_SPAN // 32, HEADS), jnp.float32, math.log(0.25), 0.0))
    entire_throughput = jnp.repeat(block_rate, 32, axis=1)
    transfer_aligned = jax.random.uniform(incomplete_key_vectors[1], tensor_dimension_count, jnp.float32) < 2.0 / CONTEXT_SPAN
    transfer_span = jnp.log(jax.random.uniform(incomplete_key_vectors[2], tensor_dimension_count, jnp.float32, 0.5, 0.8))
    forgetting_shift = -entire_throughput / CONTEXT_SPAN + jnp.where(transfer_aligned, transfer_span, 0.0)
    input_shift = jnp.clip(jax.random.normal(incomplete_key_vectors[3], tensor_dimension_count, jnp.float32), -6.0, 6.0)
    return jnp.stack([input_shift, forgetting_shift], axis=2).astype(jnp.float32)


def shard_levels(key, extent, cuts, low, high):
    def one(dim, shards_of):
        steps = jax.random.uniform(jax.random.fold_in(jax.random.fold_in(key, 6), dim), (shards_of,), jnp.float32, low / len(cuts), high / len(cuts))
        return jnp.repeat(jnp.exp(steps), extent[dim] // shards_of).reshape((-1,) + (1,) * (len(extent) - dim - 1))

    level = one(*cuts[0])
    for cut in cuts[1:]:
        level = level * one(*cut)
    return level


def noise(rng, extent, spread, bound, cuts=(), dtype=jnp.bfloat16):
    factor_of = shard_levels(rng, extent, cuts, -0.22, 0.18) if cuts else 1.0
    result = jax.random.normal(rng, extent, jnp.float32) * spread * factor_of
    return jnp.minimum(jnp.maximum(result, -bound), bound).astype(dtype)


def setup_inputs(seed: int = 0, part: int = 0) -> dict:
    seeds = jax.random.split(jax.random.key(seed), 11)
    part_keys = jax.random.split(jax.random.fold_in(seeds[10], part), 11)
    tokens = noise(part_keys[0], (SEQS, CONTEXT_SPAN, D), 1.0, 6.0, ((1, 8),))
    new_rows = noise(part_keys[1], (SEQS, D), 1.0, 6.0)
    new_query = noise(part_keys[2], (SEQS, HEADS * DK), 1.0, 6.0, ((1, 2),))
    norm_gain = jnp.clip(1.0 + 0.18 * jax.random.normal(seeds[3], (D,), jnp.float32), 0.099609375, 1.8984375).astype(jnp.bfloat16)
    key_weight = noise(seeds[4], (D, HEADS * DK), D ** -0.5, 0.125, ((0, 8), (1, 2)))
    value_weight = noise(seeds[5], (D, HEADS * DV), D ** -0.5, 0.125, ((0, 8), (1, 2)))
    input_weight = noise(seeds[6], (D, HEADS), D ** -0.5, 0.125)
    forget_weight = noise(seeds[7], (D, HEADS), D ** -0.5, 0.125)
    forget_bias = draw_forget_bias(jax.random.fold_in(seeds[10], 71), part)
    gate_offsets = draw_gate_offsets(jax.random.fold_in(jax.random.fold_in(seeds[10], part), 71), part)
    return {"tokens": tokens, "new_rows": new_rows, "new_query": new_query, "norm_gain": norm_gain, "key_weight": key_weight, "value_weight": value_weight, "input_weight": input_weight, "forget_weight": forget_weight, "forget_bias": forget_bias, "gate_offsets": gate_offsets}


EPSILON = 1e-06

def normed_rows(source, norm_gain):
    widened = source.astype(jnp.float32)
    inverse_rms = lax.rsqrt(lax.optimization_barrier(jnp.mean(widened * widened, axis=-1, keepdims=True)) + EPSILON)
    return (widened * inverse_rms * norm_gain.astype(jnp.float32)).astype(jnp.bfloat16)

def suffix_sums(log_forget):
    flipped = jnp.cumsum(jnp.flip(log_forget, 1), axis=1)
    return jnp.flip(flipped, 1) - log_forget

def cache_order(rows):
    width = rows.shape[-1]
    split = rows.reshape(SEQS, N_SP, PIECES, SUB, width)
    return jnp.transpose(split, (0, 2, 1, 3, 4)).reshape(SEQS * PIECES, N_SP * SUB, width)

def reference(tokens, new_rows, new_query, norm_gain, key_weight, value_weight, input_weight, forget_weight, forget_bias, gate_offsets):
    seq_count = tokens.shape[0]
    flat_rows = normed_rows(tokens, norm_gain).reshape(seq_count * CONTEXT_SPAN, D)
    key_rows = (jnp.dot(flat_rows, key_weight, preferred_element_type=jnp.float32) * DK ** (-0.5)).astype(jnp.bfloat16)
    value_rows = jnp.dot(flat_rows, value_weight, preferred_element_type=jnp.float32).astype(jnp.bfloat16)
    input_gate = jnp.dot(flat_rows, input_weight, preferred_element_type=jnp.float32).reshape(seq_count, CONTEXT_SPAN, HEADS) + gate_offsets[:, :, 0, :]
    forget_pre = jnp.dot(flat_rows, forget_weight, preferred_element_type=jnp.float32).reshape(seq_count, CONTEXT_SPAN, HEADS)
    log_forget = jax.nn.log_sigmoid(forget_pre + forget_bias) + gate_offsets[:, :, 1, :]
    log_weight = input_gate + suffix_sums(log_forget)
    peak_log = lax.optimization_barrier(jnp.max(log_weight, axis=1))
    query_heads = new_query.reshape(seq_count, HEADS, DK).astype(jnp.float32)
    key_heads = key_rows.reshape(seq_count, CONTEXT_SPAN, HEADS, DK).astype(jnp.float32)
    value_heads = value_rows.reshape(seq_count, CONTEXT_SPAN, HEADS, DV).astype(jnp.float32)
    scores = jnp.einsum('nhd,nshd->nsh', query_heads, key_heads)
    weighted_terms = jnp.exp(log_weight - peak_log[:, None, :]) * scores
    rounded = lax.optimization_barrier(weighted_terms.astype(jnp.bfloat16)).astype(jnp.float32)
    numerator = jnp.einsum('nsh,nshd->nhd', rounded, value_heads)
    denominator = lax.optimization_barrier(jnp.sum(weighted_terms, axis=1))
    fresh_rows = normed_rows(new_rows, norm_gain)
    key_new = (jnp.dot(fresh_rows, key_weight, preferred_element_type=jnp.float32) * DK ** (-0.5)).astype(jnp.bfloat16)
    value_new = jnp.dot(fresh_rows, value_weight, preferred_element_type=jnp.float32).astype(jnp.bfloat16)
    gate_new = jnp.dot(fresh_rows, input_weight, preferred_element_type=jnp.float32)
    peak_new = jnp.maximum(peak_log, gate_new)
    old_part = jnp.exp(peak_log - peak_new)
    own_score = jnp.einsum('nhd,nhd->nh', query_heads, key_new.reshape(seq_count, HEADS, DK).astype(jnp.float32))
    new_part = jnp.exp(gate_new - peak_new) * own_score
    total_value = old_part[..., None] * numerator + new_part[..., None] * value_new.reshape(seq_count, HEADS, DV).astype(jnp.float32)
    total_weight = old_part * denominator + new_part
    read_out = total_value / jnp.maximum(jnp.abs(total_weight), 1.0)[..., None]
    return (cache_order(key_rows.reshape(seq_count, CONTEXT_SPAN, HEADS * DK)), cache_order(value_rows.reshape(seq_count, CONTEXT_SPAN, HEADS * DV)), jnp.transpose(cache_order(log_weight), (0, 2, 1)), read_out.reshape(seq_count, HEADS * DV).astype(jnp.bfloat16))
```

```python
import jax
import jax.numpy as jnp
from jax import lax
from jax.sharding import PartitionSpec as P

EPSILON = 1e-06
HIGHEST = lax.Precision.HIGHEST


def normed_rows(source, norm_gain):
    widened = source.astype(jnp.float32)
    inverse_rms = lax.rsqrt(jnp.mean(widened * widened, axis=-1, keepdims=True) + EPSILON)
    return (widened * inverse_rms * norm_gain.astype(jnp.float32)).astype(jnp.bfloat16)


def contract_last(a, b):
    return lax.dot_general(a, b, (((1,), (1,)), ((), ())), preferred_element_type=jnp.float32)


def log_weights(gates, offsets, forget_bias, heads, blocks, pieces):
    rows = gates.shape[1]
    sub = rows // blocks
    input_gate = gates[:heads] + offsets[:heads]
    log_forget = jax.nn.log_sigmoid(gates[heads:] + forget_bias[:, None]) + offsets[heads:]
    by_block = log_forget.reshape(heads, blocks, sub)
    later = jnp.tril(jnp.ones((sub, sub), jnp.float32), -1)
    within = jnp.dot(by_block.reshape(heads * blocks, sub), later, precision=HIGHEST)
    totals = jnp.sum(by_block, axis=2)
    index = lax.axis_index("sp")
    everything = lax.all_gather(totals, "sp")
    ours = lax.dynamic_slice_in_dim(everything, index // pieces * pieces, pieces, 0)
    piece = index % pieces
    all_pieces = jnp.sum(ours, axis=0)
    after = jnp.flip(jnp.cumsum(jnp.flip(all_pieces, 1), axis=1), 1) - all_pieces
    follows = (jnp.arange(pieces) > piece).astype(jnp.float32)
    after = after + jnp.sum(ours * follows[:, None, None], axis=0)
    suffix = within.reshape(heads, blocks, sub) + after[:, :, None]
    return input_gate + suffix.reshape(heads, rows)


def read_part(query, keys, values, log_weight, heads):
    key_size = keys.shape[1] // heads
    value_size = values.shape[1] // heads
    peak = jnp.max(log_weight, axis=1, keepdims=True)
    own_head = jnp.arange(heads)[:, None] == jnp.arange(keys.shape[1])[None, :] // key_size
    spread = jnp.where(own_head, query, jnp.zeros_like(query))
    scores = contract_last(spread, keys)
    terms = jnp.exp(log_weight - peak) * scores
    wide = jnp.dot(terms.astype(jnp.bfloat16), values, preferred_element_type=jnp.float32)
    pick = jnp.eye(heads, dtype=jnp.float32)
    numerator = jnp.sum(wide.reshape(heads, heads, value_size) * pick[:, :, None], axis=1)
    return peak, numerator, jnp.sum(terms, axis=1, keepdims=True)


def finish(peak, numerator, denominator, own_score, gate_new, value_new, seq_count, pieces):
    heads, value_size = numerator.shape
    one = jnp.concatenate([peak, denominator, own_score, gate_new], axis=1)
    one = jnp.pad(one, ((0, 0), (0, value_size - one.shape[1])))
    packed = jnp.concatenate([numerator, value_new, one], axis=1)
    everything = lax.all_gather(packed, "sp").reshape(seq_count, pieces, heads, -1)
    one = everything[..., 2 * value_size :]
    peaks, denominators = one[..., 0], one[..., 1]
    own_score, gate_new = one[:, 0, :, 2], one[:, 0, :, 3]
    value_new = everything[:, 0, :, value_size : 2 * value_size]
    top = jnp.maximum(jnp.max(peaks, axis=1), gate_new)
    old = jnp.exp(peaks - top[:, None])
    new = jnp.exp(gate_new - top) * own_score
    total = jnp.sum(old[..., None] * everything[..., :value_size], axis=1)
    total = total + new[..., None] * value_new
    weight = jnp.sum(old * denominators, axis=1) + new
    return total / jnp.maximum(jnp.abs(weight), 1.0)[..., None]


def per_device(
    tokens,
    new_rows,
    new_query,
    norm_gain,
    key_weight,
    value_weight,
    input_weight,
    forget_weight,
    forget_bias,
    gate_offsets,
):
    seq_count, positions, model_width = tokens.shape
    heads = forget_bias.shape[0]
    key_size = key_weight.shape[1] // heads
    group = lax.axis_size("sp")
    shares = lax.axis_size("tp")
    pieces = group // seq_count
    sub = positions // pieces
    rows = group * sub
    index, core = lax.axis_index("sp"), lax.axis_index("tp")
    prompt = index // pieces

    part = model_width // shares
    mine = lax.dynamic_slice_in_dim(tokens.reshape(group, sub, model_width), core * part, part, 2)
    moved = lax.all_to_all(mine, "sp", split_axis=0, concat_axis=0, tiled=True)
    source = lax.all_gather(moved.reshape(rows, part), "tp", axis=1, tiled=True)
    offsets = jnp.transpose(gate_offsets.reshape(group, sub, 2 * heads), (0, 2, 1))
    offsets = lax.all_to_all(offsets, "sp", split_axis=0, concat_axis=0, tiled=True)
    offsets = jnp.transpose(offsets, (1, 0, 2)).reshape(2 * heads, rows)
    key_weight = lax.all_gather(key_weight, "sp", axis=0, tiled=True)
    value_weight = lax.all_gather(value_weight, "sp", axis=0, tiled=True)

    normed = normed_rows(source, norm_gain)
    fresh = normed_rows(lax.dynamic_slice_in_dim(new_rows, prompt, 1, 0), norm_gain)
    head_start = core * heads
    gate_weight = jnp.concatenate(
        [
            lax.dynamic_slice_in_dim(input_weight, head_start, heads, 1),
            lax.dynamic_slice_in_dim(forget_weight, head_start, heads, 1),
        ],
        axis=1,
    ).T
    gates = contract_last(gate_weight, normed)
    gate_new = contract_last(gate_weight[:heads], fresh)

    def project(x):
        keys = jnp.dot(x, key_weight, preferred_element_type=jnp.float32) * key_size**-0.5
        values = jnp.dot(x, value_weight, preferred_element_type=jnp.float32)
        return keys.astype(jnp.bfloat16), values.astype(jnp.bfloat16)

    keys, values = project(normed)
    key_new, value_new = project(fresh)
    log_weight = log_weights(gates, offsets, forget_bias, heads, group, pieces)
    query = lax.dynamic_slice_in_dim(new_query, prompt, 1, 0)
    peak, numerator, denominator = read_part(query, keys, values, log_weight, heads)
    own_score = jnp.sum(
        (query.astype(jnp.float32) * key_new.astype(jnp.float32)).reshape(heads, key_size),
        axis=1,
        keepdims=True,
    )
    value_new = value_new.astype(jnp.float32).reshape(heads, -1)
    read_out = finish(
        peak, numerator, denominator, own_score, gate_new, value_new, seq_count, pieces
    )
    return (
        keys[None],
        values[None],
        log_weight[None],
        read_out.reshape(seq_count, -1).astype(jnp.bfloat16),
    )


def solution(mesh):
    return jax.shard_map(
        per_device,
        mesh=mesh,
        in_specs=(
            P("gr", "sp", None),
            P("gr", None),
            P("gr", "tp"),
            P(),
            P("sp", "tp"),
            P("sp", "tp"),
            P(),
            P(),
            P("tp"),
            P("gr", "sp", None, "tp"),
        ),
        out_specs=(
            P(("gr", "sp"), None, "tp"),
            P(("gr", "sp"), None, "tp"),
            P(("gr", "sp"), "tp", None),
            P("gr", "tp"),
        ),
        check_vma=False,
    )
```

```python
import functools

import jax
import jax.numpy as jnp
from jax import lax
from jax.experimental import pallas as pl
from jax.experimental.pallas import tpu as pltpu
from jax.sharding import PartitionSpec as P

EPSILON = 1e-06
HIGHEST = lax.Precision.HIGHEST


def normed_rows(source, norm_gain):
    widened = source.astype(jnp.float32)
    inverse_rms = lax.rsqrt(jnp.mean(widened * widened, axis=-1, keepdims=True) + EPSILON)
    return (widened * inverse_rms * norm_gain.astype(jnp.float32)).astype(jnp.bfloat16)


def contract_last(a, b):
    return lax.dot_general(a, b, (((1,), (1,)), ((), ())), preferred_element_type=jnp.float32)


def log_weights(gates, offsets, forget_bias, heads, blocks, pieces):
    rows = gates.shape[1]
    sub = rows // blocks
    input_gate = gates[:heads] + offsets[:heads]
    log_forget = jax.nn.log_sigmoid(gates[heads:] + forget_bias[:, None]) + offsets[heads:]
    by_block = log_forget.reshape(heads, blocks, sub)
    later = jnp.tril(jnp.ones((sub, sub), jnp.float32), -1)
    within = jnp.dot(by_block.reshape(heads * blocks, sub), later, precision=HIGHEST)
    totals = jnp.sum(by_block, axis=2)
    index = lax.axis_index("sp")
    everything = lax.all_gather(totals, "sp")
    ours = lax.dynamic_slice_in_dim(everything, index // pieces * pieces, pieces, 0)
    piece = index % pieces
    all_pieces = jnp.sum(ours, axis=0)
    after = jnp.flip(jnp.cumsum(jnp.flip(all_pieces, 1), axis=1), 1) - all_pieces
    follows = (jnp.arange(pieces) > piece).astype(jnp.float32)
    after = after + jnp.sum(ours * follows[:, None, None], axis=0)
    suffix = within.reshape(heads, blocks, sub) + after[:, :, None]
    return input_gate + suffix.reshape(heads, rows)


def read_part(query, keys, values, log_weight, heads):
    key_size = keys.shape[1] // heads
    value_size = values.shape[1] // heads
    peak = jnp.max(log_weight, axis=1, keepdims=True)
    own_head = jnp.arange(heads)[:, None] == jnp.arange(keys.shape[1])[None, :] // key_size
    spread = jnp.where(own_head, query, jnp.zeros_like(query))
    scores = contract_last(spread, keys)
    terms = jnp.exp(log_weight - peak) * scores
    wide = jnp.dot(terms.astype(jnp.bfloat16), values, preferred_element_type=jnp.float32)
    pick = jnp.eye(heads, dtype=jnp.float32)
    numerator = jnp.sum(wide.reshape(heads, heads, value_size) * pick[:, :, None], axis=1)
    return peak, numerator, jnp.sum(terms, axis=1, keepdims=True)


def finish(peak, numerator, denominator, own_score, gate_new, value_new, seq_count, pieces):
    heads, value_size = numerator.shape
    one = jnp.concatenate([peak, denominator, own_score, gate_new], axis=1)
    one = jnp.pad(one, ((0, 0), (0, value_size - one.shape[1])))
    packed = jnp.concatenate([numerator, value_new, one], axis=1)
    everything = lax.all_gather(packed, "sp").reshape(seq_count, pieces, heads, -1)
    one = everything[..., 2 * value_size :]
    peaks, denominators = one[..., 0], one[..., 1]
    own_score, gate_new = one[:, 0, :, 2], one[:, 0, :, 3]
    value_new = everything[:, 0, :, value_size : 2 * value_size]
    top = jnp.maximum(jnp.max(peaks, axis=1), gate_new)
    old = jnp.exp(peaks - top[:, None])
    new = jnp.exp(gate_new - top) * own_score
    total = jnp.sum(old[..., None] * everything[..., :value_size], axis=1)
    total = total + new[..., None] * value_new
    weight = jnp.sum(old * denominators, axis=1) + new
    return total / jnp.maximum(jnp.abs(weight), 1.0)[..., None]


def line_width(group):
    width = 1
    while width * width * 4 <= group:
        width *= 2
    return width


def move_and_project(
    sizes,
    tokens,
    weight,
    offsets,
    new_rows,
    norm_gain,
    gate_weight,
    keys_out,
    values_out,
    gates_out,
    offsets_out,
    fresh_out,
    held_weight,
    held_tokens,
    normed,
    local_sem,
    z_send,
    z_recv,
    y_send,
    y_recv,
    x_send,
    x_recv,
    t_send,
    t_recv,
    f_send,
    f_recv,
    o_send,
    o_recv,
):
    depth, width, groups, shares, scale = sizes
    group = depth * width
    sub, model_width = tokens.shape[1:]
    part = model_width // shares
    x, s, c = lax.axis_index("gr"), lax.axis_index("sp"), lax.axis_index("tp")
    z, y = s // width, s % width

    def wrap(value, size):
        return lax.rem(value, size)

    barrier = pltpu.get_barrier_semaphore()
    partners = [{"sp": wrap(s + k, group)} for k in range(1, group)]
    partners += [{"gr": wrap(x + k, groups)} for k in range(1, groups)]
    partners += [{"tp": wrap(c + k, shares)} for k in range(1, shares)]
    for partner in partners:
        pl.semaphore_signal(barrier, inc=1, device_id=partner, device_id_type=pl.DeviceIdType.MESH)
    pl.semaphore_wait(barrier, len(partners))

    def remote(src, dst, send, recv, to):
        return pltpu.make_async_remote_copy(
            src_ref=src,
            dst_ref=dst,
            send_sem=send,
            recv_sem=recv,
            device_id=to,
            device_id_type=pl.DeviceIdType.MESH,
        )

    def piece(zz, yy, xx, own=False):
        return weight.at[xx] if own else held_weight.at[zz * width + yy, xx]

    def along_z(zz, way, own=False):
        return remote(
            piece(zz, y, x, own),
            held_weight.at[zz * width + y, x],
            z_send.at[zz, way],
            z_recv.at[zz],
            {"sp": s + (width if way else -width)},
        )

    def along_y(zz, k, own=False):
        return remote(
            piece(zz, y, x, own),
            held_weight.at[zz * width + y, x],
            y_send.at[zz, k],
            y_recv.at[zz, y],
            {"sp": z * width + wrap(y + k, width)},
        )

    def along_x(zz, yy, k):
        return remote(
            held_weight.at[zz * width + yy, x],
            held_weight.at[zz * width + yy, x],
            x_send.at[zz * width + yy, k],
            x_recv.at[zz * width + yy, x],
            {"gr": wrap(x + k, groups)},
        )

    def got_z(zz):
        ref = held_weight.at[zz * width + y, x]
        remote(ref, ref, z_send.at[zz, 0], z_recv.at[zz], {"sp": s}).wait_recv()

    def got_y(zz, yy):
        ref = held_weight.at[zz * width + yy, x]
        remote(ref, ref, y_send.at[zz, 0], y_recv.at[zz, yy], {"sp": s}).wait_recv()

    def got_x(ss, xx):
        ref = held_weight.at[ss, xx]
        remote(ref, ref, x_send.at[ss, 0], x_recv.at[ss, xx], {"sp": s}).wait_recv()

    columns = pl.ds(pl.multiple_of(c * part, part), part)

    def send_block(to):
        return remote(
            tokens.at[to, :, columns],
            held_tokens.at[s, :, columns],
            t_send.at[to],
            t_recv.at[s],
            {"sp": to},
        )

    def send_offsets(to):
        return remote(
            offsets.at[to], offsets_out.at[s], o_send.at[to], o_recv.at[s], {"sp": to}
        )

    def forward_block(source, k):
        return remote(
            held_tokens.at[source, :, columns],
            held_tokens.at[source, :, columns],
            f_send.at[source, k],
            f_recv.at[source, c],
            {"tp": wrap(c + k, shares)},
        )

    def got_block(source):
        ref = held_tokens.at[source, :, columns]
        remote(ref, ref, t_send.at[source], t_recv.at[source], {"sp": s}).wait_recv()

    def got_forward(source, k):
        cc = wrap(c + k, shares)
        at = pl.ds(pl.multiple_of(cc * part, part), part)
        ref = held_tokens.at[source, :, at]
        remote(ref, ref, f_send.at[source, 0], f_recv.at[source, cc], {"sp": s}).wait_recv()

    def got_offsets(source):
        ref = offsets_out.at[source]
        remote(ref, ref, o_send.at[source], o_recv.at[source], {"sp": s}).wait_recv()

    def sides(d, body):
        for way in (1, 0):
            zz = z - d if way else z + d
            pl.when((zz >= 0) & (zz < depth))(functools.partial(body, zz, way))

    def z_onward(zz, way, run, own=False):
        there = z + (1 if way else -1)

        @pl.when((there >= 0) & (there < depth))
        def _():
            run(along_z(zz, way, own))

    start = lambda copy: copy.start()

    def tokens_at(distance, run):
        def one(zz, way):
            for k in range(width):
                run(zz * width + wrap(y + k, width))

        if distance:
            sides(distance, one)
        else:
            for k in range(1, width):
                run(z * width + wrap(y + k, width))

    own_weight = pltpu.make_async_copy(weight, held_weight.at[s], local_sem.at[0])
    own_tokens = pltpu.make_async_copy(tokens.at[s], held_tokens.at[s], local_sem.at[1])
    own_offsets = pltpu.make_async_copy(offsets.at[s], offsets_out.at[s], local_sem.at[2])
    for way in (1, 0):
        z_onward(z, way, start, True)
    for k in range(1, width):
        along_y(z, k, True).start()
    for k in range(1, group):
        send_offsets(wrap(s + k, group)).start()
    own_weight.start()
    own_tokens.start()
    own_offsets.start()
    tokens_at(0, lambda to: send_block(to).start())

    def y_pieces(zz, way):
        for k in range(1, width):
            yy = wrap(y + k, width)
            got_y(zz, yy)
            for kk in range(1, groups):
                along_x(zz, yy, kk).start()

    def z_pieces(zz, way):
        got_z(zz)
        z_onward(zz, way, start)
        for k in range(1, width):
            along_y(zz, k).start()
        for k in range(1, groups):
            along_x(zz, y, k).start()

    for d in range(1, depth):
        sides(d, z_pieces)
        tokens_at(depth - d, lambda to: send_block(to).start())
        if d == 1:
            y_pieces(z, 1)
        else:
            sides(d - 1, y_pieces)
    sides(depth - 1, y_pieces)

    def norm(rows):
        wide = rows.astype(jnp.float32)
        mean = jnp.mean(wide * wide, axis=-1, keepdims=True)
        gain = norm_gain[...].astype(jnp.float32)
        return (wide * lax.rsqrt(mean + EPSILON) * gain).astype(jnp.bfloat16)

    def norm_block(source):
        at = pl.ds(pl.multiple_of(source * sub, sub), sub)
        normed[at, :] = norm(held_tokens[source])

    def order(body):
        tokens_at(0, body)
        for d in range(depth - 1, 0, -1):
            tokens_at(d, body)

    fresh = norm(new_rows[...])
    own_tokens.wait()
    norm_block(s)

    def pass_on(source):
        got_block(source)
        for k in range(1, shares):
            forward_block(source, k).start()

    def take(source):
        for k in range(1, shares):
            got_forward(source, k)
        norm_block(source)

    order(pass_on)
    order(take)
    own_weight.wait()
    for k in range(1, group):
        for kk in range(1, groups):
            got_x(wrap(s + k, group), wrap(x + kk, groups))

    key_columns, value_columns = keys_out.shape[1], values_out.shape[1]
    rows = normed.shape[0]
    tall = min(rows, 512)

    gates_out[...] = jnp.dot(normed[...], gate_weight[...], preferred_element_type=jnp.float32)
    total = key_columns + value_columns
    fresh_out[:, total:] = jnp.dot(fresh, gate_weight[...], preferred_element_type=jnp.float32)

    def project(out, first, factor):
        wide = 256 if out.shape[1] % 256 == 0 else 128

        @pl.loop(0, out.shape[1] // wide)
        def _(n):
            at = pl.ds(pl.multiple_of(n * wide, wide), wide)
            from_at = pl.ds(pl.multiple_of(first + n * wide, wide if first % wide == 0 else 128), wide)
            w = held_weight[:, :, :, from_at].reshape(model_width, wide)
            new = jnp.dot(fresh, w, preferred_element_type=jnp.float32)
            fresh_out[:, from_at] = new * factor
            for m in range(rows // tall):
                lines = pl.ds(m * tall, tall)
                got = jnp.dot(normed[lines, :], w, preferred_element_type=jnp.float32)
                out[lines, at] = (got * factor).astype(out.dtype)

    project(keys_out, 0, scale)
    project(values_out, key_columns, 1.0)

    own_offsets.wait()
    for k in range(1, group):
        got_offsets(wrap(s + k, group))

    for way in (1, 0):
        z_onward(z, way, lambda copy: copy.wait_send(), True)
    for k in range(1, width):
        along_y(z, k, True).wait_send()
    for k in range(1, group):
        to = wrap(s + k, group)
        send_offsets(to).wait_send()
        send_block(to).wait_send()
        for kk in range(1, shares):
            forward_block(to, kk).wait_send()
        for kk in range(1, groups):
            along_x(to // width, to % width, kk).wait_send()

    def sent_z(zz, way):
        z_onward(zz, way, lambda copy: copy.wait_send())
        for k in range(1, width):
            along_y(zz, k).wait_send()

    for d in range(1, depth):
        sides(d, sent_z)


def gather_and_project(tokens, weight, offsets, new_rows, norm_gain, gate_weight, key_columns, scale):
    group, sub, model_width = tokens.shape
    width = line_width(group)
    depth = group // width
    groups, shares = lax.axis_size("gr"), lax.axis_size("tp")
    total = weight.shape[1]
    rows = group * sub
    sizes = (depth, width, groups, shares, scale)
    share = weight.shape[0] // groups
    dma = pltpu.SemaphoreType.DMA
    vmem = pl.BlockSpec(memory_space=pltpu.VMEM)
    hbm = pl.BlockSpec(memory_space=pl.ANY)
    lanes = gate_weight.shape[1]
    return pl.pallas_call(
        functools.partial(move_and_project, sizes),
        name="move_and_project",
        out_shape=(
            jax.ShapeDtypeStruct((rows, key_columns), jnp.bfloat16),
            jax.ShapeDtypeStruct((rows, total - key_columns), jnp.bfloat16),
            jax.ShapeDtypeStruct((rows, lanes), jnp.float32),
            jax.ShapeDtypeStruct(offsets.shape, jnp.float32),
            jax.ShapeDtypeStruct((new_rows.shape[0], total + lanes), jnp.float32),
        ),
        in_specs=[hbm, hbm, hbm, vmem, vmem, vmem],
        out_specs=(vmem, vmem, vmem, vmem, vmem),
        scratch_shapes=[
            pltpu.VMEM((group, groups, share, total), jnp.bfloat16),
            pltpu.VMEM((group, sub, model_width), jnp.bfloat16),
            pltpu.VMEM((rows, model_width), jnp.bfloat16),
            dma((3,)),
            dma((depth, 2)),
            dma((depth,)),
            dma((depth, width)),
            dma((depth, width)),
            dma((group, groups)),
            dma((group, groups)),
            dma((group,)),
            dma((group,)),
            dma((group, shares)),
            dma((group, shares)),
            dma((group,)),
            dma((group,)),
        ],
        compiler_params=pltpu.CompilerParams(
            collective_id=0, has_side_effects=True, vmem_limit_bytes=48 * 1024 * 1024
        ),
    )(tokens, weight.reshape(groups, share, total), offsets, new_rows, norm_gain, gate_weight)


def per_device(
    tokens,
    new_rows,
    new_query,
    norm_gain,
    key_weight,
    value_weight,
    input_weight,
    forget_weight,
    forget_bias,
    gate_offsets,
):
    seq_count, positions, model_width = tokens.shape
    heads = forget_bias.shape[0]
    key_size = key_weight.shape[1] // heads
    group = lax.axis_size("sp")
    pieces = group // seq_count
    sub = positions // pieces
    rows = group * sub
    index, core = lax.axis_index("sp"), lax.axis_index("tp")
    prompt = index // pieces

    offsets = jnp.transpose(gate_offsets.reshape(group, sub, 2 * heads), (0, 2, 1))
    weight = jnp.concatenate([key_weight, value_weight], axis=1)
    head_start = core * heads
    gate_weight = jnp.concatenate(
        [
            lax.dynamic_slice_in_dim(input_weight, head_start, heads, 1),
            lax.dynamic_slice_in_dim(forget_weight, head_start, heads, 1),
        ],
        axis=1,
    )
    gate_weight = jnp.pad(gate_weight, ((0, 0), (0, -2 * heads % 128)))
    key_columns = key_weight.shape[1]
    keys, values, gates, offsets, fresh = gather_and_project(
        tokens.reshape(group, sub, model_width),
        weight,
        offsets,
        jnp.pad(new_rows, ((0, -seq_count % 16), (0, 0))),
        norm_gain[None],
        gate_weight,
        key_columns,
        key_size**-0.5,
    )
    gates = gates[:, : 2 * heads].T
    offsets = jnp.transpose(offsets, (1, 0, 2)).reshape(2 * heads, rows)
    fresh = lax.dynamic_slice_in_dim(fresh, prompt, 1, 0)
    total = weight.shape[1]
    key_new = fresh[:, :key_columns].astype(jnp.bfloat16)
    value_new = fresh[:, key_columns:total].astype(jnp.bfloat16)
    gate_new = fresh[:, total : total + heads].reshape(heads, 1)
    log_weight = log_weights(gates, offsets, forget_bias, heads, group, pieces)
    query = lax.dynamic_slice_in_dim(new_query, prompt, 1, 0)
    peak, numerator, denominator = read_part(query, keys, values, log_weight, heads)
    own_score = jnp.sum(
        (query.astype(jnp.float32) * key_new.astype(jnp.float32)).reshape(heads, key_size),
        axis=1,
        keepdims=True,
    )
    value_new = value_new.astype(jnp.float32).reshape(heads, -1)
    read_out = finish(
        peak, numerator, denominator, own_score, gate_new, value_new, seq_count, pieces
    )
    return (
        keys[None],
        values[None],
        log_weight[None],
        read_out.reshape(seq_count, -1).astype(jnp.bfloat16),
    )


def solution(mesh):
    return jax.shard_map(
        per_device,
        mesh=mesh,
        in_specs=(
            P("gr", "sp", None),
            P("gr", None),
            P("gr", "tp"),
            P(),
            P("sp", "tp"),
            P("sp", "tp"),
            P(),
            P(),
            P("tp"),
            P("gr", "sp", None, "tp"),
        ),
        out_specs=(
            P(("gr", "sp"), None, "tp"),
            P(("gr", "sp"), None, "tp"),
            P(("gr", "sp"), "tp", None),
            P("gr", "tp"),
        ),
        check_vma=False,
    )
```

```python
import functools

import jax
import jax.numpy as jnp
from jax import lax
from jax.experimental import pallas as pl
from jax.experimental.pallas import tpu as pltpu
from jax.sharding import PartitionSpec as P

EPSILON = 1e-06
HIGHEST = lax.Precision.HIGHEST


def normed_rows(source, norm_gain):
    widened = source.astype(jnp.float32)
    inverse_rms = lax.rsqrt(jnp.mean(widened * widened, axis=-1, keepdims=True) + EPSILON)
    return (widened * inverse_rms * norm_gain.astype(jnp.float32)).astype(jnp.bfloat16)


def contract_last(a, b):
    return lax.dot_general(a, b, (((1,), (1,)), ((), ())), preferred_element_type=jnp.float32)


def exchange_kernel(group, mine, everyone, send, recv, local):
    s = lax.axis_index("sp")
    mesh_id = pl.DeviceIdType.MESH
    barrier = pltpu.get_barrier_semaphore()
    for k in range(1, group):
        to = {"sp": lax.rem(s + k, group)}
        pl.semaphore_signal(barrier, inc=1, device_id=to, device_id_type=mesh_id)
    own = pltpu.make_async_copy(mine, everyone.at[s], local)
    own.start()
    pl.semaphore_wait(barrier, group - 1)

    def copy(k, slot):
        return pltpu.make_async_remote_copy(
            src_ref=mine,
            dst_ref=everyone.at[slot],
            send_sem=send.at[k],
            recv_sem=recv.at[slot],
            device_id={"sp": lax.rem(s + k, group)},
            device_id_type=mesh_id,
        )

    for k in range(1, group):
        copy(k, s).start()
    for k in range(1, group):
        copy(k, lax.rem(s + k, group)).wait_recv()
    for k in range(1, group):
        copy(k, s).wait_send()
    own.wait()


def gather_small(mine, name, number):
    group = lax.axis_size("sp")
    return pl.pallas_call(
        functools.partial(exchange_kernel, group),
        name=name,
        out_shape=jax.ShapeDtypeStruct((group,) + mine.shape, mine.dtype),
        in_specs=[pl.BlockSpec(memory_space=pl.ANY)],
        out_specs=pl.BlockSpec(memory_space=pl.ANY),
        scratch_shapes=[
            pltpu.SemaphoreType.DMA((group,)),
            pltpu.SemaphoreType.DMA((group,)),
            pltpu.SemaphoreType.DMA,
        ],
        compiler_params=pltpu.CompilerParams(collective_id=number, has_side_effects=True),
    )(mine)


def log_weights(gates, offsets, forget_bias, heads, blocks, pieces):
    rows = gates.shape[1]
    sub = rows // blocks
    input_gate = gates[:heads] + offsets[:heads]
    log_forget = jax.nn.log_sigmoid(gates[heads:] + forget_bias[:, None]) + offsets[heads:]
    by_block = log_forget.reshape(heads, blocks, sub)
    later = jnp.tril(jnp.ones((sub, sub), jnp.float32), -1)
    within = jnp.dot(by_block.reshape(heads * blocks, sub), later, precision=HIGHEST)
    totals = jnp.sum(by_block, axis=2)
    index = lax.axis_index("sp")
    everything = gather_small(totals, "gather_totals", 1)
    ours = lax.dynamic_slice_in_dim(everything, index // pieces * pieces, pieces, 0)
    piece = index % pieces
    all_pieces = jnp.sum(ours, axis=0)
    after = jnp.flip(jnp.cumsum(jnp.flip(all_pieces, 1), axis=1), 1) - all_pieces
    follows = (jnp.arange(pieces) > piece).astype(jnp.float32)
    after = after + jnp.sum(ours * follows[:, None, None], axis=0)
    suffix = within.reshape(heads, blocks, sub) + after[:, :, None]
    return input_gate + suffix.reshape(heads, rows)


def read_part(query, keys, values, log_weight, heads):
    key_size = keys.shape[1] // heads
    value_size = values.shape[1] // heads
    peak = jnp.max(log_weight, axis=1, keepdims=True)
    own_head = jnp.arange(heads)[:, None] == jnp.arange(keys.shape[1])[None, :] // key_size
    spread = jnp.where(own_head, query, jnp.zeros_like(query))
    scores = contract_last(spread, keys)
    terms = jnp.exp(log_weight - peak) * scores
    wide = jnp.dot(terms.astype(jnp.bfloat16), values, preferred_element_type=jnp.float32)
    pick = jnp.eye(heads, dtype=jnp.float32)
    numerator = jnp.sum(wide.reshape(heads, heads, value_size) * pick[:, :, None], axis=1)
    return peak, numerator, jnp.sum(terms, axis=1, keepdims=True)


def finish(peak, numerator, denominator, own_score, gate_new, value_new, seq_count, pieces):
    heads, value_size = numerator.shape
    one = jnp.concatenate([peak, denominator, own_score, gate_new], axis=1)
    one = jnp.pad(one, ((0, 0), (0, value_size - one.shape[1])))
    packed = jnp.concatenate([numerator, value_new, one], axis=1)
    everything = gather_small(packed, "gather_read", 2).reshape(seq_count, pieces, heads, -1)
    one = everything[..., 2 * value_size :]
    peaks, denominators = one[..., 0], one[..., 1]
    own_score, gate_new = one[:, 0, :, 2], one[:, 0, :, 3]
    value_new = everything[:, 0, :, value_size : 2 * value_size]
    top = jnp.maximum(jnp.max(peaks, axis=1), gate_new)
    old = jnp.exp(peaks - top[:, None])
    new = jnp.exp(gate_new - top) * own_score
    total = jnp.sum(old[..., None] * everything[..., :value_size], axis=1)
    total = total + new[..., None] * value_new
    weight = jnp.sum(old * denominators, axis=1) + new
    return total / jnp.maximum(jnp.abs(weight), 1.0)[..., None]


def line_width(group):
    width = 1
    while width * width * 4 <= group:
        width *= 2
    return width


def move_and_project(
    sizes,
    tokens,
    weight,
    offsets,
    new_rows,
    norm_gain,
    gate_weight,
    keys_out,
    values_out,
    gates_out,
    offsets_out,
    fresh_out,
    held_weight,
    held_tokens,
    normed,
    local_sem,
    z_send,
    z_recv,
    y_send,
    y_recv,
    x_send,
    x_recv,
    t_send,
    t_recv,
    f_send,
    f_recv,
    o_send,
    o_recv,
):
    depth, width, groups, shares, scale = sizes
    group = depth * width
    sub, model_width = tokens.shape[1:]
    part = model_width // shares
    x, s, c = lax.axis_index("gr"), lax.axis_index("sp"), lax.axis_index("tp")
    z, y = s // width, s % width

    def wrap(value, size):
        return lax.rem(value, size)

    barrier = pltpu.get_barrier_semaphore()
    partners = [{"sp": wrap(s + k, group)} for k in range(1, group)]
    partners += [{"gr": wrap(x + k, groups)} for k in range(1, groups)]
    partners += [{"tp": wrap(c + k, shares)} for k in range(1, shares)]
    for partner in partners:
        pl.semaphore_signal(barrier, inc=1, device_id=partner, device_id_type=pl.DeviceIdType.MESH)
    pl.semaphore_wait(barrier, len(partners))

    def remote(src, dst, send, recv, to):
        return pltpu.make_async_remote_copy(
            src_ref=src,
            dst_ref=dst,
            send_sem=send,
            recv_sem=recv,
            device_id=to,
            device_id_type=pl.DeviceIdType.MESH,
        )

    def piece(zz, yy, xx, own=False):
        return weight.at[xx] if own else held_weight.at[zz * width + yy, xx]

    def along_z(zz, way, own=False):
        return remote(
            piece(zz, y, x, own),
            held_weight.at[zz * width + y, x],
            z_send.at[zz, way],
            z_recv.at[zz],
            {"sp": s + (width if way else -width)},
        )

    def along_y(zz, k, own=False):
        return remote(
            piece(zz, y, x, own),
            held_weight.at[zz * width + y, x],
            y_send.at[zz, k],
            y_recv.at[zz, y],
            {"sp": z * width + wrap(y + k, width)},
        )

    def along_x(zz, yy, k):
        return remote(
            held_weight.at[zz * width + yy, x],
            held_weight.at[zz * width + yy, x],
            x_send.at[zz * width + yy, k],
            x_recv.at[zz * width + yy, x],
            {"gr": wrap(x + k, groups)},
        )

    def got_z(zz):
        ref = held_weight.at[zz * width + y, x]
        remote(ref, ref, z_send.at[zz, 0], z_recv.at[zz], {"sp": s}).wait_recv()

    def got_y(zz, yy):
        ref = held_weight.at[zz * width + yy, x]
        remote(ref, ref, y_send.at[zz, 0], y_recv.at[zz, yy], {"sp": s}).wait_recv()

    def got_x(ss, xx):
        ref = held_weight.at[ss, xx]
        remote(ref, ref, x_send.at[ss, 0], x_recv.at[ss, xx], {"sp": s}).wait_recv()

    columns = pl.ds(pl.multiple_of(c * part, part), part)

    def send_block(to):
        return remote(
            tokens.at[to, :, columns],
            held_tokens.at[s, :, columns],
            t_send.at[to],
            t_recv.at[s],
            {"sp": to},
        )

    def send_offsets(to):
        return remote(
            offsets.at[to], offsets_out.at[s], o_send.at[to], o_recv.at[s], {"sp": to}
        )

    def forward_block(source, k):
        return remote(
            held_tokens.at[source, :, columns],
            held_tokens.at[source, :, columns],
            f_send.at[source, k],
            f_recv.at[source, c],
            {"tp": wrap(c + k, shares)},
        )

    def got_block(source):
        ref = held_tokens.at[source, :, columns]
        remote(ref, ref, t_send.at[source], t_recv.at[source], {"sp": s}).wait_recv()

    def got_forward(source, k):
        cc = wrap(c + k, shares)
        at = pl.ds(pl.multiple_of(cc * part, part), part)
        ref = held_tokens.at[source, :, at]
        remote(ref, ref, f_send.at[source, 0], f_recv.at[source, cc], {"sp": s}).wait_recv()

    def got_offsets(source):
        ref = offsets_out.at[source]
        remote(ref, ref, o_send.at[source], o_recv.at[source], {"sp": s}).wait_recv()

    def sides(d, body):
        for way in (1, 0):
            zz = z - d if way else z + d
            pl.when((zz >= 0) & (zz < depth))(functools.partial(body, zz, way))

    def z_onward(zz, way, run, own=False):
        there = z + (1 if way else -1)

        @pl.when((there >= 0) & (there < depth))
        def _():
            run(along_z(zz, way, own))

    start = lambda copy: copy.start()

    def tokens_at(distance, run):
        def one(zz, way):
            for k in range(width):
                run(zz * width + wrap(y + k, width))

        if distance:
            sides(distance, one)
        else:
            for k in range(1, width):
                run(z * width + wrap(y + k, width))

    own_weight = pltpu.make_async_copy(weight, held_weight.at[s], local_sem.at[0])
    own_tokens = pltpu.make_async_copy(tokens.at[s], held_tokens.at[s], local_sem.at[1])
    own_offsets = pltpu.make_async_copy(offsets.at[s], offsets_out.at[s], local_sem.at[2])
    for way in (1, 0):
        z_onward(z, way, start, True)
    for k in range(1, width):
        along_y(z, k, True).start()
    for k in range(1, group):
        send_offsets(wrap(s + k, group)).start()
    own_weight.start()
    own_tokens.start()
    own_offsets.start()
    tokens_at(0, lambda to: send_block(to).start())

    def y_pieces(zz, way):
        for k in range(1, width):
            yy = wrap(y + k, width)
            got_y(zz, yy)
            for kk in range(1, groups):
                along_x(zz, yy, kk).start()

    def z_pieces(zz, way):
        got_z(zz)
        z_onward(zz, way, start)
        for k in range(1, width):
            along_y(zz, k).start()
        for k in range(1, groups):
            along_x(zz, y, k).start()

    for d in range(1, depth):
        sides(d, z_pieces)
        tokens_at(depth - d, lambda to: send_block(to).start())
        if d == 1:
            y_pieces(z, 1)
        else:
            sides(d - 1, y_pieces)
    sides(depth - 1, y_pieces)

    def norm(rows):
        wide = rows.astype(jnp.float32)
        mean = jnp.mean(wide * wide, axis=-1, keepdims=True)
        gain = norm_gain[...].astype(jnp.float32)
        return (wide * lax.rsqrt(mean + EPSILON) * gain).astype(jnp.bfloat16)

    def norm_block(source):
        at = pl.ds(pl.multiple_of(source * sub, sub), sub)
        normed[at, :] = norm(held_tokens[source])

    def order(body):
        tokens_at(0, body)
        for d in range(depth - 1, 0, -1):
            tokens_at(d, body)

    fresh = norm(new_rows[...])
    own_tokens.wait()
    norm_block(s)

    def pass_on(source):
        got_block(source)
        for k in range(1, shares):
            forward_block(source, k).start()

    def take(source):
        for k in range(1, shares):
            got_forward(source, k)
        norm_block(source)

    order(pass_on)
    order(take)
    own_weight.wait()
    for k in range(1, group):
        for kk in range(1, groups):
            got_x(wrap(s + k, group), wrap(x + kk, groups))

    key_columns, value_columns = keys_out.shape[1], values_out.shape[1]
    rows = normed.shape[0]
    tall = min(rows, 512)

    gates_out[...] = jnp.dot(normed[...], gate_weight[...], preferred_element_type=jnp.float32)
    total = key_columns + value_columns
    fresh_out[:, total:] = jnp.dot(fresh, gate_weight[...], preferred_element_type=jnp.float32)

    def project(out, first, factor):
        wide = 256 if out.shape[1] % 256 == 0 else 128

        @pl.loop(0, out.shape[1] // wide)
        def _(n):
            at = pl.ds(pl.multiple_of(n * wide, wide), wide)
            from_at = pl.ds(pl.multiple_of(first + n * wide, wide if first % wide == 0 else 128), wide)
            w = held_weight[:, :, :, from_at].reshape(model_width, wide)
            new = jnp.dot(fresh, w, preferred_element_type=jnp.float32)
            fresh_out[:, from_at] = new * factor
            for m in range(rows // tall):
                lines = pl.ds(m * tall, tall)
                got = jnp.dot(normed[lines, :], w, preferred_element_type=jnp.float32)
                out[lines, at] = (got * factor).astype(out.dtype)

    project(keys_out, 0, scale)
    project(values_out, key_columns, 1.0)

    own_offsets.wait()
    for k in range(1, group):
        got_offsets(wrap(s + k, group))

    for way in (1, 0):
        z_onward(z, way, lambda copy: copy.wait_send(), True)
    for k in range(1, width):
        along_y(z, k, True).wait_send()
    for k in range(1, group):
        to = wrap(s + k, group)
        send_offsets(to).wait_send()
        send_block(to).wait_send()
        for kk in range(1, shares):
            forward_block(to, kk).wait_send()
        for kk in range(1, groups):
            along_x(to // width, to % width, kk).wait_send()

    def sent_z(zz, way):
        z_onward(zz, way, lambda copy: copy.wait_send())
        for k in range(1, width):
            along_y(zz, k).wait_send()

    for d in range(1, depth):
        sides(d, sent_z)


def gather_and_project(tokens, weight, offsets, new_rows, norm_gain, gate_weight, key_columns, scale):
    group, sub, model_width = tokens.shape
    width = line_width(group)
    depth = group // width
    groups, shares = lax.axis_size("gr"), lax.axis_size("tp")
    total = weight.shape[1]
    rows = group * sub
    sizes = (depth, width, groups, shares, scale)
    share = weight.shape[0] // groups
    dma = pltpu.SemaphoreType.DMA
    vmem = pl.BlockSpec(memory_space=pltpu.VMEM)
    hbm = pl.BlockSpec(memory_space=pl.ANY)
    lanes = gate_weight.shape[1]
    return pl.pallas_call(
        functools.partial(move_and_project, sizes),
        name="move_and_project",
        out_shape=(
            jax.ShapeDtypeStruct((rows, key_columns), jnp.bfloat16),
            jax.ShapeDtypeStruct((rows, total - key_columns), jnp.bfloat16),
            jax.ShapeDtypeStruct((rows, lanes), jnp.float32),
            jax.ShapeDtypeStruct(offsets.shape, jnp.float32),
            jax.ShapeDtypeStruct((new_rows.shape[0], total + lanes), jnp.float32),
        ),
        in_specs=[hbm, hbm, hbm, vmem, vmem, vmem],
        out_specs=(vmem, vmem, vmem, vmem, vmem),
        scratch_shapes=[
            pltpu.VMEM((group, groups, share, total), jnp.bfloat16),
            pltpu.VMEM((group, sub, model_width), jnp.bfloat16),
            pltpu.VMEM((rows, model_width), jnp.bfloat16),
            dma((3,)),
            dma((depth, 2)),
            dma((depth,)),
            dma((depth, width)),
            dma((depth, width)),
            dma((group, groups)),
            dma((group, groups)),
            dma((group,)),
            dma((group,)),
            dma((group, shares)),
            dma((group, shares)),
            dma((group,)),
            dma((group,)),
        ],
        compiler_params=pltpu.CompilerParams(
            collective_id=0, has_side_effects=True, vmem_limit_bytes=48 * 1024 * 1024
        ),
    )(tokens, weight.reshape(groups, share, total), offsets, new_rows, norm_gain, gate_weight)


def per_device(
    tokens,
    new_rows,
    new_query,
    norm_gain,
    key_weight,
    value_weight,
    input_weight,
    forget_weight,
    forget_bias,
    gate_offsets,
):
    seq_count, positions, model_width = tokens.shape
    heads = forget_bias.shape[0]
    key_size = key_weight.shape[1] // heads
    group = lax.axis_size("sp")
    pieces = group // seq_count
    sub = positions // pieces
    rows = group * sub
    index, core = lax.axis_index("sp"), lax.axis_index("tp")
    prompt = index // pieces

    offsets = jnp.transpose(gate_offsets.reshape(group, sub, 2 * heads), (0, 2, 1))
    weight = jnp.concatenate([key_weight, value_weight], axis=1)
    head_start = core * heads
    gate_weight = jnp.concatenate(
        [
            lax.dynamic_slice_in_dim(input_weight, head_start, heads, 1),
            lax.dynamic_slice_in_dim(forget_weight, head_start, heads, 1),
        ],
        axis=1,
    )
    gate_weight = jnp.pad(gate_weight, ((0, 0), (0, -2 * heads % 128)))
    key_columns = key_weight.shape[1]
    keys, values, gates, offsets, fresh = gather_and_project(
        tokens.reshape(group, sub, model_width),
        weight,
        offsets,
        jnp.pad(new_rows, ((0, -seq_count % 16), (0, 0))),
        norm_gain[None],
        gate_weight,
        key_columns,
        key_size**-0.5,
    )
    gates = gates[:, : 2 * heads].T
    offsets = jnp.transpose(offsets, (1, 0, 2)).reshape(2 * heads, rows)
    fresh = lax.dynamic_slice_in_dim(fresh, prompt, 1, 0)
    total = weight.shape[1]
    key_new = fresh[:, :key_columns].astype(jnp.bfloat16)
    value_new = fresh[:, key_columns:total].astype(jnp.bfloat16)
    gate_new = fresh[:, total : total + heads].reshape(heads, 1)
    log_weight = log_weights(gates, offsets, forget_bias, heads, group, pieces)
    query = lax.dynamic_slice_in_dim(new_query, prompt, 1, 0)
    peak, numerator, denominator = read_part(query, keys, values, log_weight, heads)
    own_score = jnp.sum(
        (query.astype(jnp.float32) * key_new.astype(jnp.float32)).reshape(heads, key_size),
        axis=1,
        keepdims=True,
    )
    value_new = value_new.astype(jnp.float32).reshape(heads, -1)
    read_out = finish(
        peak, numerator, denominator, own_score, gate_new, value_new, seq_count, pieces
    )
    return (
        keys[None],
        values[None],
        log_weight[None],
        read_out.reshape(seq_count, -1).astype(jnp.bfloat16),
    )


def solution(mesh):
    return jax.shard_map(
        per_device,
        mesh=mesh,
        in_specs=(
            P("gr", "sp", None),
            P("gr", None),
            P("gr", "tp"),
            P(),
            P("sp", "tp"),
            P("sp", "tp"),
            P(),
            P(),
            P("tp"),
            P("gr", "sp", None, "tp"),
        ),
        out_specs=(
            P(("gr", "sp"), None, "tp"),
            P(("gr", "sp"), None, "tp"),
            P(("gr", "sp"), "tp", None),
            P("gr", "tp"),
        ),
        check_vma=False,
    )
```

```python
import functools

import jax
import jax.numpy as jnp
from jax import lax
from jax.experimental import pallas as pl
from jax.experimental.pallas import tpu as pltpu
from jax.sharding import PartitionSpec as P

EPSILON = 1e-06
HIGHEST = lax.Precision.HIGHEST


def normed_rows(source, norm_gain):
    widened = source.astype(jnp.float32)
    inverse_rms = lax.rsqrt(jnp.mean(widened * widened, axis=-1, keepdims=True) + EPSILON)
    return (widened * inverse_rms * norm_gain.astype(jnp.float32)).astype(jnp.bfloat16)


def contract_last(a, b):
    return lax.dot_general(a, b, (((1,), (1,)), ((), ())), preferred_element_type=jnp.float32)


def exchange_kernel(group, mine, everyone, send, recv, local):
    s = lax.axis_index("sp")
    mesh_id = pl.DeviceIdType.MESH
    barrier = pltpu.get_barrier_semaphore()
    for k in range(1, group):
        to = {"sp": lax.rem(s + k, group)}
        pl.semaphore_signal(barrier, inc=1, device_id=to, device_id_type=mesh_id)
    own = pltpu.make_async_copy(mine, everyone.at[s], local)
    own.start()
    pl.semaphore_wait(barrier, group - 1)

    def copy(k, slot):
        return pltpu.make_async_remote_copy(
            src_ref=mine,
            dst_ref=everyone.at[slot],
            send_sem=send.at[k],
            recv_sem=recv.at[slot],
            device_id={"sp": lax.rem(s + k, group)},
            device_id_type=mesh_id,
        )

    for k in range(1, group):
        copy(k, s).start()
    for k in range(1, group):
        copy(k, lax.rem(s + k, group)).wait_recv()
    for k in range(1, group):
        copy(k, s).wait_send()
    own.wait()


def gather_small(mine, name, number):
    group = lax.axis_size("sp")
    return pl.pallas_call(
        functools.partial(exchange_kernel, group),
        name=name,
        out_shape=jax.ShapeDtypeStruct((group,) + mine.shape, mine.dtype),
        in_specs=[pl.BlockSpec(memory_space=pl.ANY)],
        out_specs=pl.BlockSpec(memory_space=pl.ANY),
        scratch_shapes=[
            pltpu.SemaphoreType.DMA((group,)),
            pltpu.SemaphoreType.DMA((group,)),
            pltpu.SemaphoreType.DMA,
        ],
        compiler_params=pltpu.CompilerParams(collective_id=number, has_side_effects=True),
    )(mine)


def log_weights(gates, offsets, forget_bias, totals, heads, blocks, pieces):
    rows = gates.shape[1]
    sub = rows // blocks
    input_gate = gates[:heads] + offsets[:heads]
    log_forget = jax.nn.log_sigmoid(gates[heads:] + forget_bias[:, None]) + offsets[heads:]
    by_block = log_forget.reshape(heads, blocks, sub)
    later = jnp.tril(jnp.ones((sub, sub), jnp.float32), -1)
    within = jnp.dot(by_block.reshape(heads * blocks, sub), later, precision=HIGHEST)
    index = lax.axis_index("sp")
    everything = totals[:, :, :blocks]
    ours = lax.dynamic_slice_in_dim(everything, index // pieces * pieces, pieces, 0)
    piece = index % pieces
    all_pieces = jnp.sum(ours, axis=0)
    after = jnp.flip(jnp.cumsum(jnp.flip(all_pieces, 1), axis=1), 1) - all_pieces
    follows = (jnp.arange(pieces) > piece).astype(jnp.float32)
    after = after + jnp.sum(ours * follows[:, None, None], axis=0)
    suffix = within.reshape(heads, blocks, sub) + after[:, :, None]
    return input_gate + suffix.reshape(heads, rows)


def read_part(query, keys, values, log_weight, heads):
    key_size = keys.shape[1] // heads
    value_size = values.shape[1] // heads
    peak = jnp.max(log_weight, axis=1, keepdims=True)
    own_head = jnp.arange(heads)[:, None] == jnp.arange(keys.shape[1])[None, :] // key_size
    spread = jnp.where(own_head, query, jnp.zeros_like(query))
    scores = contract_last(spread, keys)
    terms = jnp.exp(log_weight - peak) * scores
    wide = jnp.dot(terms.astype(jnp.bfloat16), values, preferred_element_type=jnp.float32)
    pick = jnp.eye(heads, dtype=jnp.float32)
    numerator = jnp.sum(wide.reshape(heads, heads, value_size) * pick[:, :, None], axis=1)
    return peak, numerator, jnp.sum(terms, axis=1, keepdims=True)


def finish(peak, numerator, denominator, own_score, gate_new, value_new, seq_count, pieces):
    heads, value_size = numerator.shape
    one = jnp.concatenate([peak, denominator, own_score, gate_new], axis=1)
    one = jnp.pad(one, ((0, 0), (0, value_size - one.shape[1])))
    packed = jnp.concatenate([numerator, value_new, one], axis=1)
    everything = gather_small(packed, "gather_read", 2).reshape(seq_count, pieces, heads, -1)
    one = everything[..., 2 * value_size :]
    peaks, denominators = one[..., 0], one[..., 1]
    own_score, gate_new = one[:, 0, :, 2], one[:, 0, :, 3]
    value_new = everything[:, 0, :, value_size : 2 * value_size]
    top = jnp.maximum(jnp.max(peaks, axis=1), gate_new)
    old = jnp.exp(peaks - top[:, None])
    new = jnp.exp(gate_new - top) * own_score
    total = jnp.sum(old[..., None] * everything[..., :value_size], axis=1)
    total = total + new[..., None] * value_new
    weight = jnp.sum(old * denominators, axis=1) + new
    return total / jnp.maximum(jnp.abs(weight), 1.0)[..., None]


def line_width(group):
    width = 1
    while width * width * 4 <= group:
        width *= 2
    return width


def move_and_project(
    sizes,
    tokens,
    weight,
    offsets,
    new_rows,
    norm_gain,
    gate_weight,
    forget_bias,
    keys_out,
    values_out,
    gates_out,
    offsets_out,
    fresh_out,
    totals_out,
    held_weight,
    held_tokens,
    normed,
    local_sem,
    z_send,
    z_recv,
    y_send,
    y_recv,
    x_send,
    x_recv,
    t_send,
    t_recv,
    f_send,
    f_recv,
    o_send,
    o_recv,
    s_send,
    s_recv,
):
    depth, width, groups, shares, scale = sizes
    group = depth * width
    sub, model_width = tokens.shape[1:]
    part = model_width // shares
    x, s, c = lax.axis_index("gr"), lax.axis_index("sp"), lax.axis_index("tp")
    z, y = s // width, s % width

    def wrap(value, size):
        return lax.rem(value, size)

    barrier = pltpu.get_barrier_semaphore()
    partners = [{"sp": wrap(s + k, group)} for k in range(1, group)]
    partners += [{"gr": wrap(x + k, groups)} for k in range(1, groups)]
    partners += [{"tp": wrap(c + k, shares)} for k in range(1, shares)]
    for partner in partners:
        pl.semaphore_signal(barrier, inc=1, device_id=partner, device_id_type=pl.DeviceIdType.MESH)
    pl.semaphore_wait(barrier, len(partners))

    def remote(src, dst, send, recv, to):
        return pltpu.make_async_remote_copy(
            src_ref=src,
            dst_ref=dst,
            send_sem=send,
            recv_sem=recv,
            device_id=to,
            device_id_type=pl.DeviceIdType.MESH,
        )

    def piece(zz, yy, xx, own=False):
        return weight.at[xx] if own else held_weight.at[zz * width + yy, xx]

    def along_z(zz, way, own=False):
        return remote(
            piece(zz, y, x, own),
            held_weight.at[zz * width + y, x],
            z_send.at[zz, way],
            z_recv.at[zz],
            {"sp": s + (width if way else -width)},
        )

    def along_y(zz, k, own=False):
        return remote(
            piece(zz, y, x, own),
            held_weight.at[zz * width + y, x],
            y_send.at[zz, k],
            y_recv.at[zz, y],
            {"sp": z * width + wrap(y + k, width)},
        )

    def along_x(zz, yy, k):
        return remote(
            held_weight.at[zz * width + yy, x],
            held_weight.at[zz * width + yy, x],
            x_send.at[zz * width + yy, k],
            x_recv.at[zz * width + yy, x],
            {"gr": wrap(x + k, groups)},
        )

    def got_z(zz):
        ref = held_weight.at[zz * width + y, x]
        remote(ref, ref, z_send.at[zz, 0], z_recv.at[zz], {"sp": s}).wait_recv()

    def got_y(zz, yy):
        ref = held_weight.at[zz * width + yy, x]
        remote(ref, ref, y_send.at[zz, 0], y_recv.at[zz, yy], {"sp": s}).wait_recv()

    def got_x(ss, xx):
        ref = held_weight.at[ss, xx]
        remote(ref, ref, x_send.at[ss, 0], x_recv.at[ss, xx], {"sp": s}).wait_recv()

    columns = pl.ds(pl.multiple_of(c * part, part), part)

    def send_block(to):
        return remote(
            tokens.at[to, :, columns],
            held_tokens.at[s, :, columns],
            t_send.at[to],
            t_recv.at[s],
            {"sp": to},
        )

    def send_offsets(to):
        return remote(
            offsets.at[to], offsets_out.at[s], o_send.at[to], o_recv.at[s], {"sp": to}
        )

    def send_totals(to, slot):
        ref = totals_out.at[slot]
        return remote(ref, ref, s_send.at[to], s_recv.at[slot], {"sp": to})

    def forward_block(source, k):
        return remote(
            held_tokens.at[source, :, columns],
            held_tokens.at[source, :, columns],
            f_send.at[source, k],
            f_recv.at[source, c],
            {"tp": wrap(c + k, shares)},
        )

    def got_block(source):
        ref = held_tokens.at[source, :, columns]
        remote(ref, ref, t_send.at[source], t_recv.at[source], {"sp": s}).wait_recv()

    def got_forward(source, k):
        cc = wrap(c + k, shares)
        at = pl.ds(pl.multiple_of(cc * part, part), part)
        ref = held_tokens.at[source, :, at]
        remote(ref, ref, f_send.at[source, 0], f_recv.at[source, cc], {"sp": s}).wait_recv()

    def got_offsets(source):
        ref = offsets_out.at[source]
        remote(ref, ref, o_send.at[source], o_recv.at[source], {"sp": s}).wait_recv()

    def sides(d, body):
        for way in (1, 0):
            zz = z - d if way else z + d
            pl.when((zz >= 0) & (zz < depth))(functools.partial(body, zz, way))

    def z_onward(zz, way, run, own=False):
        there = z + (1 if way else -1)

        @pl.when((there >= 0) & (there < depth))
        def _():
            run(along_z(zz, way, own))

    start = lambda copy: copy.start()

    def tokens_at(distance, run):
        def one(zz, way):
            for k in range(width):
                run(zz * width + wrap(y + k, width))

        if distance:
            sides(distance, one)
        else:
            for k in range(1, width):
                run(z * width + wrap(y + k, width))

    own_weight = pltpu.make_async_copy(weight, held_weight.at[s], local_sem.at[0])
    own_tokens = pltpu.make_async_copy(tokens.at[s], held_tokens.at[s], local_sem.at[1])
    own_offsets = pltpu.make_async_copy(offsets.at[s], offsets_out.at[s], local_sem.at[2])
    for way in (1, 0):
        z_onward(z, way, start, True)
    for k in range(1, width):
        along_y(z, k, True).start()
    for k in range(1, group):
        send_offsets(wrap(s + k, group)).start()
    own_weight.start()
    own_tokens.start()
    own_offsets.start()
    tokens_at(0, lambda to: send_block(to).start())

    def y_pieces(zz, way):
        for k in range(1, width):
            yy = wrap(y + k, width)
            got_y(zz, yy)
            for kk in range(1, groups):
                along_x(zz, yy, kk).start()

    def z_pieces(zz, way):
        got_z(zz)
        z_onward(zz, way, start)
        for k in range(1, width):
            along_y(zz, k).start()
        for k in range(1, groups):
            along_x(zz, y, k).start()

    for d in range(1, depth):
        sides(d, z_pieces)
        tokens_at(depth - d, lambda to: send_block(to).start())
        if d == 1:
            y_pieces(z, 1)
        else:
            sides(d - 1, y_pieces)
    sides(depth - 1, y_pieces)

    def norm(rows):
        wide = rows.astype(jnp.float32)
        mean = jnp.mean(wide * wide, axis=-1, keepdims=True)
        gain = norm_gain[...].astype(jnp.float32)
        return (wide * lax.rsqrt(mean + EPSILON) * gain).astype(jnp.bfloat16)

    def norm_block(source):
        at = pl.ds(pl.multiple_of(source * sub, sub), sub)
        normed[at, :] = norm(held_tokens[source])

    def order(body):
        tokens_at(0, body)
        for d in range(depth - 1, 0, -1):
            tokens_at(d, body)

    fresh = norm(new_rows[...])
    own_tokens.wait()
    norm_block(s)

    def pass_on(source):
        got_block(source)
        for k in range(1, shares):
            forward_block(source, k).start()

    def take(source):
        for k in range(1, shares):
            got_forward(source, k)
        norm_block(source)

    order(pass_on)
    order(take)
    own_offsets.wait()
    for k in range(1, group):
        got_offsets(wrap(s + k, group))

    heads = forget_bias.shape[0]
    gates = jnp.dot(normed[...], gate_weight[...], preferred_element_type=jnp.float32).T
    gates_out[...] = gates[: gates_out.shape[0]]
    lane = lax.broadcasted_iota(jnp.int32, (heads, totals_out.shape[2]), 1)
    totals = jnp.zeros((heads, totals_out.shape[2]), jnp.float32)
    for j in range(group):
        pre = gates[heads : 2 * heads, j * sub : (j + 1) * sub] + forget_bias[...]
        log_forget = jnp.minimum(pre, 0.0) - jnp.log1p(jnp.exp(-jnp.abs(pre)))
        log_forget = log_forget + offsets_out[j, heads : 2 * heads, :]
        block_total = jnp.sum(log_forget, axis=1, keepdims=True)
        totals = totals + jnp.where(lane == j, block_total, 0.0)
    totals_out[s] = totals

    own_weight.wait()
    for k in range(1, group):
        for kk in range(1, groups):
            got_x(wrap(s + k, group), wrap(x + kk, groups))

    key_columns, value_columns = keys_out.shape[1], values_out.shape[1]
    rows = normed.shape[0]
    tall = min(rows, 512)

    for k in range(1, group):
        send_totals(wrap(s + k, group), s).start()
    total = key_columns + value_columns
    fresh_out[:, total:] = jnp.dot(fresh, gate_weight[...], preferred_element_type=jnp.float32)

    def project(out, first, factor):
        wide = 256 if out.shape[1] % 256 == 0 else 128

        @pl.loop(0, out.shape[1] // wide)
        def _(n):
            at = pl.ds(pl.multiple_of(n * wide, wide), wide)
            from_at = pl.ds(pl.multiple_of(first + n * wide, wide if first % wide == 0 else 128), wide)
            w = held_weight[:, :, :, from_at].reshape(model_width, wide)
            new = jnp.dot(fresh, w, preferred_element_type=jnp.float32)
            fresh_out[:, from_at] = new * factor
            for m in range(rows // tall):
                lines = pl.ds(m * tall, tall)
                got = jnp.dot(normed[lines, :], w, preferred_element_type=jnp.float32)
                out[lines, at] = (got * factor).astype(out.dtype)

    project(keys_out, 0, scale)
    project(values_out, key_columns, 1.0)

    for k in range(1, group):
        other = wrap(s + k, group)
        send_totals(other, other).wait_recv()

    for way in (1, 0):
        z_onward(z, way, lambda copy: copy.wait_send(), True)
    for k in range(1, width):
        along_y(z, k, True).wait_send()
    for k in range(1, group):
        to = wrap(s + k, group)
        send_offsets(to).wait_send()
        send_totals(to, s).wait_send()
        send_block(to).wait_send()
        for kk in range(1, shares):
            forward_block(to, kk).wait_send()
        for kk in range(1, groups):
            along_x(to // width, to % width, kk).wait_send()

    def sent_z(zz, way):
        z_onward(zz, way, lambda copy: copy.wait_send())
        for k in range(1, width):
            along_y(zz, k).wait_send()

    for d in range(1, depth):
        sides(d, sent_z)


def gather_and_project(tokens, weight, offsets, new_rows, norm_gain, gate_weight, forget_bias, key_columns, scale):
    group, sub, model_width = tokens.shape
    width = line_width(group)
    depth = group // width
    groups, shares = lax.axis_size("gr"), lax.axis_size("tp")
    total = weight.shape[1]
    rows = group * sub
    sizes = (depth, width, groups, shares, scale)
    share = weight.shape[0] // groups
    dma = pltpu.SemaphoreType.DMA
    vmem = pl.BlockSpec(memory_space=pltpu.VMEM)
    hbm = pl.BlockSpec(memory_space=pl.ANY)
    lanes = gate_weight.shape[1]
    return pl.pallas_call(
        functools.partial(move_and_project, sizes),
        name="move_and_project",
        out_shape=(
            jax.ShapeDtypeStruct((rows, key_columns), jnp.bfloat16),
            jax.ShapeDtypeStruct((rows, total - key_columns), jnp.bfloat16),
            jax.ShapeDtypeStruct((offsets.shape[1], rows), jnp.float32),
            jax.ShapeDtypeStruct(offsets.shape, jnp.float32),
            jax.ShapeDtypeStruct((new_rows.shape[0], total + lanes), jnp.float32),
            jax.ShapeDtypeStruct((group, forget_bias.shape[0], 128), jnp.float32),
        ),
        in_specs=[hbm, hbm, hbm, vmem, vmem, vmem, vmem],
        out_specs=(vmem, vmem, vmem, vmem, vmem, vmem),
        scratch_shapes=[
            pltpu.VMEM((group, groups, share, total), jnp.bfloat16),
            pltpu.VMEM((group, sub, model_width), jnp.bfloat16),
            pltpu.VMEM((rows, model_width), jnp.bfloat16),
            dma((3,)),
            dma((depth, 2)),
            dma((depth,)),
            dma((depth, width)),
            dma((depth, width)),
            dma((group, groups)),
            dma((group, groups)),
            dma((group,)),
            dma((group,)),
            dma((group, shares)),
            dma((group, shares)),
            dma((group,)),
            dma((group,)),
            dma((group,)),
            dma((group,)),
        ],
        compiler_params=pltpu.CompilerParams(
            collective_id=0, has_side_effects=True, vmem_limit_bytes=48 * 1024 * 1024
        ),
    )(tokens, weight.reshape(groups, share, total), offsets, new_rows, norm_gain, gate_weight, forget_bias)


def per_device(
    tokens,
    new_rows,
    new_query,
    norm_gain,
    key_weight,
    value_weight,
    input_weight,
    forget_weight,
    forget_bias,
    gate_offsets,
):
    seq_count, positions, model_width = tokens.shape
    heads = forget_bias.shape[0]
    key_size = key_weight.shape[1] // heads
    group = lax.axis_size("sp")
    pieces = group // seq_count
    sub = positions // pieces
    rows = group * sub
    index, core = lax.axis_index("sp"), lax.axis_index("tp")
    prompt = index // pieces

    offsets = jnp.transpose(gate_offsets.reshape(group, sub, 2 * heads), (0, 2, 1))
    weight = jnp.concatenate([key_weight, value_weight], axis=1)
    head_start = core * heads
    gate_weight = jnp.concatenate(
        [
            lax.dynamic_slice_in_dim(input_weight, head_start, heads, 1),
            lax.dynamic_slice_in_dim(forget_weight, head_start, heads, 1),
        ],
        axis=1,
    )
    gate_weight = jnp.pad(gate_weight, ((0, 0), (0, -2 * heads % 128)))
    key_columns = key_weight.shape[1]
    keys, values, gates, offsets, fresh, totals = gather_and_project(
        tokens.reshape(group, sub, model_width),
        weight,
        offsets,
        jnp.pad(new_rows, ((0, -seq_count % 16), (0, 0))),
        norm_gain[None],
        gate_weight,
        forget_bias[:, None],
        key_columns,
        key_size**-0.5,
    )
    offsets = jnp.transpose(offsets, (1, 0, 2)).reshape(2 * heads, rows)
    fresh = lax.dynamic_slice_in_dim(fresh, prompt, 1, 0)
    total = weight.shape[1]
    key_new = fresh[:, :key_columns].astype(jnp.bfloat16)
    value_new = fresh[:, key_columns:total].astype(jnp.bfloat16)
    gate_new = fresh[:, total : total + heads].reshape(heads, 1)
    log_weight = log_weights(gates, offsets, forget_bias, totals, heads, group, pieces)
    query = lax.dynamic_slice_in_dim(new_query, prompt, 1, 0)
    peak, numerator, denominator = read_part(query, keys, values, log_weight, heads)
    own_score = jnp.sum(
        (query.astype(jnp.float32) * key_new.astype(jnp.float32)).reshape(heads, key_size),
        axis=1,
        keepdims=True,
    )
    value_new = value_new.astype(jnp.float32).reshape(heads, -1)
    read_out = finish(
        peak, numerator, denominator, own_score, gate_new, value_new, seq_count, pieces
    )
    return (
        keys[None],
        values[None],
        log_weight[None],
        read_out.reshape(seq_count, -1).astype(jnp.bfloat16),
    )


def solution(mesh):
    return jax.shard_map(
        per_device,
        mesh=mesh,
        in_specs=(
            P("gr", "sp", None),
            P("gr", None),
            P("gr", "tp"),
            P(),
            P("sp", "tp"),
            P("sp", "tp"),
            P(),
            P(),
            P("tp"),
            P("gr", "sp", None, "tp"),
        ),
        out_specs=(
            P(("gr", "sp"), None, "tp"),
            P(("gr", "sp"), None, "tp"),
            P(("gr", "sp"), "tp", None),
            P("gr", "tp"),
        ),
        check_vma=False,
    )
```
